32 devices in a mesh: sp: 8 (over z, y), dp: 4 (over x, core).
Axes of the slice: x: 2, y: 2, z: 4, core: 2. Of those that a mesh axis runs over, the one named last changes fastest.
Arguments:
- query: bfloat16 [4, 1536, 3072], P('dp', 'sp'), may hold values from -18 to 18
- latent: bfloat16 [4, 1536, 1024], P('dp', 'sp'), may hold values from -6 to 6
- rope_key: bfloat16 [4, 1536, 32], P('dp', 'sp'), may hold values from -5 to 5
- latent_norm_gain: float32 [1024], replicated, may hold values from 0.1 to 1.9
- key_up_matrix: bfloat16 [2048, 1024], P('dp'), may hold values from -0.1875 to 0.1875
- value_up_matrix: bfloat16 [2048, 1024], P('dp'), may hold values from -0.1875 to 0.1875
- out_grad: bfloat16 [4, 1536, 2048], P('dp', 'sp'), may hold values from -6 to 6
Outputs:
- query_grad: bfloat16 [4, 1536, 3072], P('dp', 'sp')
- latent_grad: float32 [4, 1536, 1024], P('dp', 'sp')
- rope_key_grad: float32 [4, 1536, 32], P('dp', 'sp')
- key_weight_grad: float32 [2048, 1024], P('dp')
- value_weight_grad: float32 [2048, 1024], P('dp')
- gain_grad: float32 [1024], replicated
The draws below stay inside these ranges and needn't reach their ends.
All inputs are finite; a program needn't handle non-finite values.
Results may differ from the reference program's by a relative error of at most 0.011.
Values may be sent and summed in bfloat16 or wider, within the bound.
A program may use at most 256 MiB of HBM per device.

```python
import jax
import jax.numpy as jnp
from jax import lax

ATTENTION_HEADS = 32
PLAIN_HEAD_WIDTH = 64
ROPE = 32
VALUE_HEAD_WIDTH = 64
LATENT_WIDTH = 1024
SPAN = 64
SEQUENCE_LENGTH = 1536
BATCH_SEQUENCES = 4


def draw_rope_key(key, part):
    own = jax.random.fold_in(key, 11)
    values = jnp.clip(jax.random.normal(own, (BATCH_SEQUENCES, SEQUENCE_LENGTH, ROPE), jnp.float32), -5.0, 5.0)
    return values.astype(jnp.bfloat16)


def draw_query(key, part):
    own = jax.random.fold_in(key, 23)
    shape = (BATCH_SEQUENCES, SEQUENCE_LENGTH, ATTENTION_HEADS, PLAIN_HEAD_WIDTH + ROPE)
    values = jnp.clip(jax.random.normal(own, shape, jnp.float32), -5.0, 5.0)
    return values.reshape(BATCH_SEQUENCES, SEQUENCE_LENGTH, ATTENTION_HEADS * (PLAIN_HEAD_WIDTH + ROPE)).astype(jnp.bfloat16)


def block_scale(own_key, shape, split, least, high):
    loudness, own = 1.0, jax.random.fold_in(own_key, 6)
    for axis_at, blocks in split:
        steps = jnp.exp(jax.random.uniform(jax.random.fold_in(own, axis_at), (blocks,), jnp.float32, least / len(split), high / len(split)))
        loudness = loudness * jnp.repeat(steps, shape[axis_at] // blocks).reshape([-1 if axis == axis_at else 1 for axis in range(len(shape))])
    return loudness


def centred(rng, dims, scale, reach, split=(), held_as=jnp.bfloat16):
    result = scale * jax.random.normal(rng, dims, jnp.float32)
    if split:
        result = result * block_scale(rng, dims, split, -0.22, 0.18)
    return jnp.clip(result, -reach, reach).astype(held_as)


def setup_inputs(seed: int = 0) -> dict:
    streams_of = jax.random.split(jax.random.key(seed), 8)
    query = draw_query(jax.random.fold_in(streams_of[7], 71), 0)
    latent = centred(streams_of[1], (BATCH_SEQUENCES, SEQUENCE_LENGTH, LATENT_WIDTH), 1.0, 6.0, ((0, 4), (1, 8)))
    rope_key = draw_rope_key(jax.random.fold_in(streams_of[7], 71), 0)
    latent_norm_gain = jnp.clip(1.0 + 0.18 * jax.random.normal(streams_of[3], (LATENT_WIDTH,), jnp.float32), 0.1, 1.9)
    key_up_matrix = centred(streams_of[4], (ATTENTION_HEADS * PLAIN_HEAD_WIDTH, LATENT_WIDTH), LATENT_WIDTH ** -0.5, 0.1875, ((0, 4),))
    value_up_matrix = centred(streams_of[5], (ATTENTION_HEADS * VALUE_HEAD_WIDTH, LATENT_WIDTH), LATENT_WIDTH ** -0.5, 0.1875, ((0, 4),))
    out_grad = centred(streams_of[6], (BATCH_SEQUENCES, SEQUENCE_LENGTH, ATTENTION_HEADS * VALUE_HEAD_WIDTH), 1.0, 6.0, ((0, 4), (1, 8)))
    return {"query": query, "latent": latent, "rope_key": rope_key, "latent_norm_gain": latent_norm_gain, "key_up_matrix": key_up_matrix, "value_up_matrix": value_up_matrix, "out_grad": out_grad}


eps = 1e-06
rope_base = 10000.0

def rotate(values, cosine, sine):
    half = values.shape[-1] // 2
    first = values[..., :half]
    second = values[..., half:]
    return jnp.concatenate([first * cosine - second * sine, second * cosine + first * sine], axis=-1)

def angles(length, width):
    inverse = 1.0 / rope_base ** (jnp.arange(0, width, 2, dtype=jnp.float32) / width)
    turned = jnp.arange(length, dtype=jnp.float32)[:, None] * inverse[None, :]
    return (jnp.cos(turned), jnp.sin(turned))

def reference(query, latent, rope_key, latent_norm_gain, key_up_matrix, value_up_matrix, out_grad):
    f32 = jnp.float32
    bf16 = jnp.bfloat16
    length = SEQUENCE_LENGTH
    width = PLAIN_HEAD_WIDTH + ROPE
    scale = width ** (-0.5)
    block = 512 if length % 512 == 0 else length
    cosine, sine = angles(length, ROPE)
    neg = jnp.finfo(f32).min

    def one_sequence(inputs):
        seq_query, seq_latent, seq_rope, seq_grad = inputs
        lat = seq_latent.astype(f32)
        inv_rms = lax.rsqrt(lax.optimization_barrier(jnp.mean(lat * lat, axis=-1, keepdims=True)) + eps)
        normed = lat * inv_rms
        nlat = (normed * latent_norm_gain).astype(bf16)
        key_nope = jnp.dot(nlat, key_up_matrix.T, preferred_element_type=f32).astype(bf16).reshape(length, ATTENTION_HEADS, PLAIN_HEAD_WIDTH)
        values = jnp.dot(nlat, value_up_matrix.T, preferred_element_type=f32).astype(bf16).reshape(length, ATTENTION_HEADS, VALUE_HEAD_WIDTH)
        heads_query = seq_query.reshape(length, ATTENTION_HEADS, width)
        q_nope = heads_query[:, :, :PLAIN_HEAD_WIDTH]
        q_rope = rotate(heads_query[:, :, PLAIN_HEAD_WIDTH:].astype(f32), cosine[:, None, :], sine[:, None, :]).astype(bf16)
        k_rope = rotate(seq_rope.astype(f32), cosine, sine).astype(bf16)
        d_out = seq_grad.reshape(length, ATTENTION_HEADS, VALUE_HEAD_WIDTH)
        dk_nope = jnp.zeros((length, ATTENTION_HEADS, PLAIN_HEAD_WIDTH), f32)
        dk_rope = jnp.zeros((length, ROPE), f32)
        d_vals = jnp.zeros((length, ATTENTION_HEADS, VALUE_HEAD_WIDTH), f32)
        dq_parts = []
        for begin in range(0, length, block):
            end = begin + block
            qn = q_nope[begin:end].astype(f32)
            qr = q_rope[begin:end].astype(f32)
            go = d_out[begin:end].astype(f32)
            kn = key_nope[:end].astype(f32)
            kr = k_rope[:end].astype(f32)
            vv = values[:end].astype(f32)
            scores = (jnp.einsum('qhd,khd->hqk', qn, kn) + jnp.einsum('qhd,kd->hqk', qr, kr)) * scale
            q_seg = jnp.arange(begin, end) // SPAN
            k_seg = jnp.arange(end) // SPAN
            allowed = k_seg[None, :] <= q_seg[:, None]
            scores = jnp.where(allowed[None], scores, neg)
            probs = jax.nn.softmax(scores, axis=-1)
            d_probs = jnp.einsum('qhd,khd->hqk', go, vv)
            d_scores = probs * (d_probs - lax.optimization_barrier(jnp.sum(probs * d_probs, axis=-1, keepdims=True)))
            ds_b = d_scores.astype(bf16).astype(f32)
            p_b = probs.astype(bf16).astype(f32)
            dq_n = jnp.einsum('hqk,khd->qhd', ds_b, kn) * scale
            dq_r = jnp.einsum('hqk,kd->qhd', ds_b, kr) * scale
            dq_r = rotate(dq_r, cosine[begin:end, None, :], -sine[begin:end, None, :])
            dq_parts.append(jnp.concatenate([dq_n, dq_r], axis=-1).astype(bf16))
            dk_nope = dk_nope.at[:end].add(jnp.einsum('hqk,qhd->khd', ds_b, qn) * scale)
            dk_rope = dk_rope.at[:end].add(jnp.einsum('hqk,qhd->kd', ds_b, qr) * scale)
            d_vals = d_vals.at[:end].add(jnp.einsum('hqk,qhd->khd', p_b, go))
        query_grad = jnp.concatenate(dq_parts, axis=0).reshape(length, ATTENTION_HEADS * width)
        rope_grad = rotate(dk_rope, cosine, -sine)
        dk_b = dk_nope.astype(bf16).reshape(length, ATTENTION_HEADS * PLAIN_HEAD_WIDTH)
        dv_b = d_vals.astype(bf16).reshape(length, ATTENTION_HEADS * VALUE_HEAD_WIDTH)
        d_nlat = jnp.dot(dk_b, key_up_matrix, preferred_element_type=f32) + jnp.dot(dv_b, value_up_matrix, preferred_element_type=f32)
        key_part = jnp.dot(dk_b.T, nlat, preferred_element_type=f32)
        value_part = jnp.dot(dv_b.T, nlat, preferred_element_type=f32)
        gain_part = lax.optimization_barrier(jnp.sum(d_nlat * normed, axis=0))
        scaled = d_nlat * latent_norm_gain
        latent_grad = inv_rms * (scaled - normed * lax.optimization_barrier(jnp.mean(scaled * normed, axis=-1, keepdims=True)))
        return (query_grad, latent_grad, rope_grad, key_part, value_part, gain_part)
    results = lax.map(one_sequence, (query, latent, rope_key, out_grad))
    query_grad, latent_grad, rope_grad, key_parts, value_parts, gain_parts = results
    return (query_grad, latent_grad, rope_grad, lax.optimization_barrier(jnp.sum(key_parts, axis=0)), lax.optimization_barrier(jnp.sum(value_parts, axis=0)), lax.optimization_barrier(jnp.sum(gain_parts, axis=0)))
```

```python
import functools
import math

import jax
import jax.numpy as jnp
from jax import lax
from jax.experimental import pallas as pl
from jax.experimental.pallas import tpu as pltpu
from jax.sharding import PartitionSpec as P

ATTENTION_HEADS = 32
PLAIN_HEAD_WIDTH = 64
ROPE = 32
VALUE_HEAD_WIDTH = 64
SPAN = 64
WIDTH = PLAIN_HEAD_WIDTH + ROPE
LANES = 128

eps = 1e-06
rope_base = 10000.0


def rotate(values, cosine, sine):
    half = values.shape[-1] // 2
    first = values[..., :half]
    second = values[..., half:]
    return jnp.concatenate(
        [first * cosine - second * sine, second * cosine + first * sine], axis=-1
    )


def angles(length, width):
    inverse = 1.0 / rope_base ** (jnp.arange(0, width, 2, dtype=jnp.float32) / width)
    turned = jnp.arange(length, dtype=jnp.float32)[:, None] * inverse[None, :]
    return (jnp.cos(turned), jnp.sin(turned))


NT = (((1,), (1,)), ((), ()))
NN = (((1,), (0,)), ((), ()))


def mm(a, b, dims=NN):
    return lax.dot_general(a, b, dims, preferred_element_type=jnp.float32)


def attention_kernel(
    heads, tile,
    arrived, keys, values, k_rope, cosine, sine,
    dq_out, dkv_out, dr_out,
    q_s, go_s, k_s, kt_s, v_s, s_s, dp_s, dk_s, dv_s, dq_s,
):
    f32 = jnp.float32
    bf16 = jnp.bfloat16
    length = k_rope.shape[0]
    blocks = length // tile
    scale = WIDTH ** (-0.5)
    steep = scale * math.log2(math.e)
    half = ROPE // 2
    pid = pl.program_id(0)

    for h in range(heads):
        @pl.when(pid == h)
        def _():
            raw = arrived[:, h * WIDTH : (h + 1) * WIDTH]
            turned = rotate(
                raw[:, PLAIN_HEAD_WIDTH:].astype(f32), cosine[:, :half], sine[:, :half]
            ).astype(bf16)
            q_s[...] = jnp.concatenate([raw[:, :PLAIN_HEAD_WIDTH], turned], axis=1)
            base = heads * WIDTH + h * VALUE_HEAD_WIDTH
            go_s[...] = arrived[:, base : base + VALUE_HEAD_WIDTH]
            both = jnp.concatenate(
                [keys[:, h * PLAIN_HEAD_WIDTH : (h + 1) * PLAIN_HEAD_WIDTH], k_rope[...]], axis=1
            )
            k_s[...] = both
            v_s[...] = values[:, h * VALUE_HEAD_WIDTH : (h + 1) * VALUE_HEAD_WIDTH]

    for b in range(blocks):
        kt_s[b] = k_s[b * tile : (b + 1) * tile, :].astype(f32).T.astype(bf16)
    dk_s[...] = jnp.zeros_like(dk_s)
    dv_s[...] = jnp.zeros_like(dv_s)

    key_seg = lax.broadcasted_iota(jnp.int32, (tile, tile), 0) // SPAN
    query_seg = lax.broadcasted_iota(jnp.int32, (tile, tile), 1) // SPAN

    def fold(x, op):
        return op(x.reshape(tile // 8, 8, tile), axis=0)

    def query_block(qi, _):
        rows = pl.ds(pl.multiple_of(qi * tile, tile), tile)
        q = q_s[rows, :]
        go = go_s[rows, :]

        def score(kb, peak, diagonal=False):
            at = pl.ds(pl.multiple_of(kb * tile, tile), tile)
            s = mm(k_s[at, :], q, NT)
            if diagonal:
                s = jnp.where(key_seg <= query_seg, s, -1e30)
            s_s[at, :] = s
            dp_s[at, :] = mm(v_s[at, :], go, NT)
            return jnp.maximum(peak, fold(s, jnp.max))

        peak = lax.fori_loop(0, qi, score, jnp.full((8, tile), -1e30, f32))
        peak = score(qi, peak, diagonal=True)
        top = jnp.max(peak, axis=0, keepdims=True) * steep

        def weigh(kb, carry):
            total, mixed = carry
            at = pl.ds(pl.multiple_of(kb * tile, tile), tile)
            p = jnp.exp2(s_s[at, :] * steep - top)
            s_s[at, :] = p
            return total + fold(p, jnp.sum), mixed + fold(p * dp_s[at, :], jnp.sum)

        zero = jnp.zeros((8, tile), f32)
        total, mixed = lax.fori_loop(0, qi + 1, weigh, (zero, zero))
        inverse = 1.0 / jnp.sum(total, axis=0, keepdims=True)
        delta = jnp.sum(mixed, axis=0, keepdims=True) * inverse

        dq_s[...] = jnp.zeros_like(dq_s)

        def spread(kb, _):
            at = pl.ds(pl.multiple_of(kb * tile, tile), tile)
            probs = s_s[at, :] * inverse
            ds = (probs * (dp_s[at, :] - delta)).astype(bf16)
            dv_s[at, :] += mm(probs.astype(bf16), go)
            dk_s[at, :] += mm(ds, q)
            dq_s[...] += mm(kt_s[kb], ds)
            return 0

        lax.fori_loop(0, qi + 1, spread, 0)
        dq = dq_s[...].T * scale
        back = rotate(dq[:, PLAIN_HEAD_WIDTH:], cosine[rows, :half], -sine[rows, :half])
        done = jnp.concatenate([dq[:, :PLAIN_HEAD_WIDTH], back], axis=1).astype(bf16)
        for h in range(heads):
            @pl.when(pid == h)
            def _():
                dq_out[rows, h * WIDTH : (h + 1) * WIDTH] = done
        return 0

    lax.fori_loop(0, blocks, query_block, 0)

    dk = dk_s[...] * scale
    for h in range(heads):
        @pl.when(pid == h)
        def _():
            dkv_out[:, h * PLAIN_HEAD_WIDTH : (h + 1) * PLAIN_HEAD_WIDTH] = dk[
                :, :PLAIN_HEAD_WIDTH
            ].astype(bf16)
            base = heads * PLAIN_HEAD_WIDTH + h * VALUE_HEAD_WIDTH
            dkv_out[:, base : base + VALUE_HEAD_WIDTH] = dv_s[...].astype(bf16)
            if h == 0:
                dr_out[...] = dk[:, PLAIN_HEAD_WIDTH:]
            else:
                dr_out[...] += dk[:, PLAIN_HEAD_WIDTH:]


def attend_backward(arrived, keys, values, k_rope, cosine, sine, heads):
    length = arrived.shape[0]
    tile = 256
    f32 = jnp.float32
    bf16 = jnp.bfloat16

    def whole(a):
        return pl.BlockSpec(a.shape, lambda i: (0,) * len(a.shape))

    outs = (
        jax.ShapeDtypeStruct((length, heads * WIDTH), bf16),
        jax.ShapeDtypeStruct((length, heads * (PLAIN_HEAD_WIDTH + VALUE_HEAD_WIDTH)), bf16),
        jax.ShapeDtypeStruct((length, ROPE), f32),
    )
    ins = (arrived, keys, values, k_rope, cosine, sine)
    return pl.pallas_call(
        functools.partial(attention_kernel, heads, tile),
        grid=(heads,),
        out_shape=outs,
        in_specs=[whole(a) for a in ins],
        out_specs=tuple(whole(a) for a in outs),
        scratch_shapes=[
            pltpu.VMEM((length, WIDTH), bf16),
            pltpu.VMEM((length, VALUE_HEAD_WIDTH), bf16),
            pltpu.VMEM((length, WIDTH), bf16),
            pltpu.VMEM((length // tile, WIDTH, tile), bf16),
            pltpu.VMEM((length, VALUE_HEAD_WIDTH), bf16),
            pltpu.VMEM((length, tile), f32),
            pltpu.VMEM((length, tile), f32),
            pltpu.VMEM((length, WIDTH), f32),
            pltpu.VMEM((length, VALUE_HEAD_WIDTH), f32),
            pltpu.VMEM((WIDTH, tile), f32),
        ],
        compiler_params=pltpu.CompilerParams(
            dimension_semantics=("arbitrary",), vmem_limit_bytes=56 * 1024 * 1024
        ),
        cost_estimate=pl.CostEstimate(
            flops=heads * length * length * 420, bytes_accessed=8 * length * 1024,
            transcendentals=heads * length * length // 2,
        ),
    )(*ins)


def normalise(latent):
    lat = latent.astype(jnp.float32)
    inv_rms = lax.rsqrt(jnp.mean(lat * lat, axis=-1, keepdims=True) + eps)
    return lat * inv_rms, inv_rms


def local(query, latent, rope_key, latent_norm_gain, key_up_matrix, value_up_matrix, out_grad):
    f32 = jnp.float32
    bf16 = jnp.bfloat16
    sp = lax.axis_size("sp")
    dp = lax.axis_size("dp")
    me = lax.axis_index("sp")
    tokens, channels = latent.shape[1:]
    heads = ATTENTION_HEADS // sp
    ratio = sp // dp
    piece = key_up_matrix.shape[0] // sp
    to_user = [
        (s * dp + d, (d * ratio + s // dp) * dp + s % dp) for s in range(sp) for d in range(dp)
    ]
    to_holder = [(b, a) for a, b in to_user]

    packed = jnp.concatenate(
        [
            query[0].reshape(tokens, sp, heads * WIDTH),
            out_grad[0].reshape(tokens, sp, heads * VALUE_HEAD_WIDTH),
        ],
        axis=-1,
    ).transpose(1, 0, 2)
    arrived = lax.all_to_all(packed, "sp", split_axis=0, concat_axis=0, tiled=True)
    arrived = arrived.reshape(sp * tokens, -1)

    fill = LANES - ROPE
    context = jnp.concatenate([latent[0], rope_key[0], jnp.zeros((tokens, fill), bf16)], axis=-1)
    context = lax.all_gather(context, "sp", axis=0, tiled=True)

    rows = jnp.stack(
        [
            lax.dynamic_slice_in_dim(key_up_matrix, me * piece, piece, 0),
            lax.dynamic_slice_in_dim(value_up_matrix, me * piece, piece, 0),
        ]
    )
    rows = lax.ppermute(rows, ("sp", "dp"), to_user)
    weights = lax.all_gather(rows, "dp", axis=1, tiled=True)

    length = sp * tokens
    cosine, sine = angles(length, ROPE)
    normed_all, _ = normalise(context[:, :channels])
    nlat = (normed_all * latent_norm_gain).astype(bf16)
    keys = lax.dot_general(nlat, weights[0], NT, preferred_element_type=f32).astype(bf16)
    values = lax.dot_general(nlat, weights[1], NT, preferred_element_type=f32).astype(bf16)
    k_rope = rotate(context[:, channels : channels + ROPE].astype(f32), cosine, sine).astype(bf16)

    dq, dkv, dr = attend_backward(arrived, keys, values, k_rope, cosine, sine, heads)

    returned = lax.all_to_all(
        dq.reshape(sp, tokens, heads * WIDTH), "sp", split_axis=0, concat_axis=0, tiled=True
    )
    query_grad = returned.transpose(1, 0, 2).reshape(tokens, ATTENTION_HEADS * WIDTH)

    both = weights.reshape(-1, channels)
    d_nlat_part = lax.dot_general(dkv, both, NN, preferred_element_type=f32)
    rope_part = rotate(dr, cosine, -sine)
    sums = jnp.concatenate(
        [d_nlat_part.astype(bf16), rope_part.astype(bf16), jnp.zeros((length, fill), bf16)], axis=-1
    )
    sums = lax.psum_scatter(sums, "sp", scatter_dimension=0, tiled=True)

    weight_part = lax.dot_general(
        dkv, nlat, (((0,), (0,)), ((), ())), preferred_element_type=f32
    ).astype(bf16)
    weight_part = weight_part.reshape(2, -1, channels)
    weight_sum = lax.psum_scatter(weight_part, "dp", scatter_dimension=1, tiled=True)
    weight_sum = lax.ppermute(weight_sum, ("sp", "dp"), to_holder)
    weight_grads = lax.all_gather(weight_sum, "sp", axis=1, tiled=True).astype(f32)

    gain_grad = lax.psum(jnp.sum(d_nlat_part * normed_all, axis=0), ("sp", "dp"))

    normed, inv_rms = normalise(latent[0])
    scaled = sums[:, :channels].astype(f32) * latent_norm_gain
    latent_grad = inv_rms * (scaled - normed * jnp.mean(scaled * normed, axis=-1, keepdims=True))
    rope_grad = sums[:, channels : channels + ROPE].astype(f32)
    return (
        query_grad[None],
        latent_grad[None],
        rope_grad[None],
        weight_grads[0],
        weight_grads[1],
        gain_grad,
    )


def solution(mesh):
    in_specs = (
        P("dp", "sp", None),
        P("dp", "sp", None),
        P("dp", "sp", None),
        P(),
        P("dp", None),
        P("dp", None),
        P("dp", "sp", None),
    )
    out_specs = (
        P("dp", "sp", None),
        P("dp", "sp", None),
        P("dp", "sp", None),
        P("dp", None),
        P("dp", None),
        P(),
    )
    return jax.shard_map(local, mesh=mesh, in_specs=in_specs, out_specs=out_specs, check_vma=False)
```

```python
import functools
import math

import jax
import jax.numpy as jnp
from jax import lax
from jax.experimental import pallas as pl
from jax.experimental.pallas import tpu as pltpu
from jax.sharding import PartitionSpec as P

ATTENTION_HEADS = 32
PLAIN_HEAD_WIDTH = 64
ROPE = 32
VALUE_HEAD_WIDTH = 64
SPAN = 64
WIDTH = PLAIN_HEAD_WIDTH + ROPE

eps = 1e-06
rope_base = 10000.0


def rotate(values, cosine, sine):
    half = values.shape[-1] // 2
    first = values[..., :half]
    second = values[..., half:]
    return jnp.concatenate(
        [first * cosine - second * sine, second * cosine + first * sine], axis=-1
    )


def angles(length, width):
    inverse = 1.0 / rope_base ** (jnp.arange(0, width, 2, dtype=jnp.float32) / width)
    turned = jnp.arange(length, dtype=jnp.float32)[:, None] * inverse[None, :]
    return (jnp.cos(turned), jnp.sin(turned))


NT = (((1,), (1,)), ((), ()))
NN = (((1,), (0,)), ((), ()))


def mm(a, b, dims=NN):
    return lax.dot_general(a, b, dims, preferred_element_type=jnp.float32)


def attention_kernel(
    heads, tile,
    arrived, keyvals, k_rope, cosine, sine,
    grads_out, dr_out,
    q_s, go_s, k_s, kt_s, v_s, s_s, dp_s, dk_s, dv_s, dq_s,
):
    f32 = jnp.float32
    bf16 = jnp.bfloat16
    length = k_rope.shape[0]
    blocks = length // tile
    scale = WIDTH ** (-0.5)
    steep = scale * math.log2(math.e)
    half = ROPE // 2
    pid = pl.program_id(0)

    for h in range(heads):
        @pl.when(pid == h)
        def _():
            raw = arrived[:, h * WIDTH : (h + 1) * WIDTH]
            turned = rotate(
                raw[:, PLAIN_HEAD_WIDTH:].astype(f32), cosine[:, :half], sine[:, :half]
            ).astype(bf16)
            q_s[...] = jnp.concatenate([raw[:, :PLAIN_HEAD_WIDTH], turned], axis=1)
            base = heads * WIDTH + h * VALUE_HEAD_WIDTH
            go_s[...] = arrived[:, base : base + VALUE_HEAD_WIDTH]
            both = jnp.concatenate(
                [keyvals[:, h * PLAIN_HEAD_WIDTH : (h + 1) * PLAIN_HEAD_WIDTH], k_rope[...]], axis=1
            )
            k_s[...] = both
            base = heads * PLAIN_HEAD_WIDTH + h * VALUE_HEAD_WIDTH
            v_s[...] = keyvals[:, base : base + VALUE_HEAD_WIDTH]

    for b in range(blocks):
        kt_s[b] = k_s[b * tile : (b + 1) * tile, :].astype(f32).T.astype(bf16)
    dk_s[...] = jnp.zeros_like(dk_s)
    dv_s[...] = jnp.zeros_like(dv_s)

    key_seg = lax.broadcasted_iota(jnp.int32, (tile, tile), 0) // SPAN
    query_seg = lax.broadcasted_iota(jnp.int32, (tile, tile), 1) // SPAN

    def fold(x, op):
        return op(x.reshape(tile // 8, 8, tile), axis=0)

    def query_block(qi, _):
        rows = pl.ds(pl.multiple_of(qi * tile, tile), tile)
        q = q_s[rows, :]
        go = go_s[rows, :]

        def score(kb, peak, diagonal=False):
            at = pl.ds(pl.multiple_of(kb * tile, tile), tile)
            s = mm(k_s[at, :], q, NT)
            if diagonal:
                s = jnp.where(key_seg <= query_seg, s, -1e30)
            s_s[at, :] = s
            dp_s[at, :] = mm(v_s[at, :], go, NT)
            return jnp.maximum(peak, fold(s, jnp.max))

        peak = lax.fori_loop(0, qi, score, jnp.full((8, tile), -1e30, f32))
        peak = score(qi, peak, diagonal=True)
        top = jnp.max(peak, axis=0, keepdims=True) * steep

        def weigh(kb, carry):
            total, mixed = carry
            at = pl.ds(pl.multiple_of(kb * tile, tile), tile)
            p = jnp.exp2(s_s[at, :] * steep - top)
            s_s[at, :] = p
            return total + fold(p, jnp.sum), mixed + fold(p * dp_s[at, :], jnp.sum)

        zero = jnp.zeros((8, tile), f32)
        total, mixed = lax.fori_loop(0, qi + 1, weigh, (zero, zero))
        inverse = 1.0 / jnp.sum(total, axis=0, keepdims=True)
        delta = jnp.sum(mixed, axis=0, keepdims=True) * inverse

        dq_s[...] = jnp.zeros_like(dq_s)

        def spread(kb, _):
            at = pl.ds(pl.multiple_of(kb * tile, tile), tile)
            probs = s_s[at, :] * inverse
            ds = (probs * (dp_s[at, :] - delta)).astype(bf16)
            dv_s[at, :] += mm(probs.astype(bf16), go)
            dk_s[at, :] += mm(ds, q)
            dq_s[...] += mm(kt_s[kb], ds)
            return 0

        lax.fori_loop(0, qi + 1, spread, 0)
        dq = dq_s[...].T * scale
        back = rotate(dq[:, PLAIN_HEAD_WIDTH:], cosine[rows, :half], -sine[rows, :half])
        done = jnp.concatenate([dq[:, :PLAIN_HEAD_WIDTH], back], axis=1).astype(bf16)
        for h in range(heads):
            @pl.when(pid == h)
            def _():
                grads_out[rows, h * WIDTH : (h + 1) * WIDTH] = done
        return 0

    lax.fori_loop(0, blocks, query_block, 0)

    dk = dk_s[...] * scale
    for h in range(heads):
        @pl.when(pid == h)
        def _():
            base = heads * WIDTH + h * PLAIN_HEAD_WIDTH
            grads_out[:, base : base + PLAIN_HEAD_WIDTH] = dk[:, :PLAIN_HEAD_WIDTH].astype(bf16)
            base = heads * (WIDTH + PLAIN_HEAD_WIDTH) + h * VALUE_HEAD_WIDTH
            grads_out[:, base : base + VALUE_HEAD_WIDTH] = dv_s[...].astype(bf16)
            if h == 0:
                dr_out[...] = dk[:, PLAIN_HEAD_WIDTH:]
            else:
                dr_out[...] += dk[:, PLAIN_HEAD_WIDTH:]


def attend_backward(arrived, keyvals, k_rope, cosine, sine, heads):
    length = arrived.shape[0]
    tile = 256
    f32 = jnp.float32
    bf16 = jnp.bfloat16

    def whole(a):
        return pl.BlockSpec(a.shape, lambda i: (0,) * len(a.shape))

    outs = (
        jax.ShapeDtypeStruct((length, heads * (WIDTH + PLAIN_HEAD_WIDTH + VALUE_HEAD_WIDTH)), bf16),
        jax.ShapeDtypeStruct((length, ROPE), f32),
    )
    ins = (arrived, keyvals, k_rope, cosine, sine)
    return pl.pallas_call(
        functools.partial(attention_kernel, heads, tile),
        grid=(heads,),
        out_shape=outs,
        in_specs=[whole(a) for a in ins],
        out_specs=tuple(whole(a) for a in outs),
        scratch_shapes=[
            pltpu.VMEM((length, WIDTH), bf16),
            pltpu.VMEM((length, VALUE_HEAD_WIDTH), bf16),
            pltpu.VMEM((length, WIDTH), bf16),
            pltpu.VMEM((length // tile, WIDTH, tile), bf16),
            pltpu.VMEM((length, VALUE_HEAD_WIDTH), bf16),
            pltpu.VMEM((length, tile), f32),
            pltpu.VMEM((length, tile), f32),
            pltpu.VMEM((length, WIDTH), f32),
            pltpu.VMEM((length, VALUE_HEAD_WIDTH), f32),
            pltpu.VMEM((WIDTH, tile), f32),
        ],
        compiler_params=pltpu.CompilerParams(
            dimension_semantics=("arbitrary",), vmem_limit_bytes=56 * 1024 * 1024
        ),
        cost_estimate=pl.CostEstimate(
            flops=heads * length * length * 420, bytes_accessed=8 * length * 1024,
            transcendentals=heads * length * length // 2,
        ),
    )(*ins)


def normalise(latent):
    lat = latent.astype(jnp.float32)
    inv_rms = lax.rsqrt(jnp.mean(lat * lat, axis=-1, keepdims=True) + eps)
    return lat * inv_rms, inv_rms


def local(query, latent, rope_key, latent_norm_gain, key_up_matrix, value_up_matrix, out_grad):
    f32 = jnp.float32
    bf16 = jnp.bfloat16
    sp = lax.axis_size("sp")
    dp = lax.axis_size("dp")
    tokens, channels = latent.shape[1:]
    heads = ATTENTION_HEADS // sp
    ratio = sp // dp
    to_user = [
        (s * dp + d, (d * ratio + s // dp) * dp + s % dp) for s in range(sp) for d in range(dp)
    ]
    to_holder = [(b, a) for a, b in to_user]

    rope_all = lax.all_gather(rope_key[0], "sp", axis=0, tiled=True)
    stacked = jnp.stack([key_up_matrix, value_up_matrix])
    whole = lax.all_gather(stacked, "dp", axis=1, tiled=True)
    packed = jnp.concatenate(
        [
            query[0].reshape(tokens, sp, heads * WIDTH),
            out_grad[0].reshape(tokens, sp, heads * VALUE_HEAD_WIDTH),
        ],
        axis=-1,
    ).transpose(1, 0, 2)
    packed, rope_all = lax.optimization_barrier((packed, rope_all))
    arrived = lax.all_to_all(packed, "sp", split_axis=0, concat_axis=0, tiled=True)
    arrived = arrived.reshape(sp * tokens, -1)

    normed, inv_rms = normalise(latent[0])
    nlat = (normed * latent_norm_gain).astype(bf16)
    key_cols = lax.dot_general(nlat, whole[0], NT, preferred_element_type=f32).astype(bf16)
    value_cols = lax.dot_general(nlat, whole[1], NT, preferred_element_type=f32).astype(bf16)
    keyvals = jnp.concatenate(
        [
            key_cols.reshape(tokens, sp, heads * PLAIN_HEAD_WIDTH),
            value_cols.reshape(tokens, sp, heads * VALUE_HEAD_WIDTH),
        ],
        axis=-1,
    ).transpose(1, 0, 2)
    keyvals = lax.all_to_all(keyvals, "sp", split_axis=0, concat_axis=0, tiled=True)
    keyvals = keyvals.reshape(sp * tokens, -1)

    nlat_late, whole = lax.optimization_barrier((nlat, whole))
    nlat_all = lax.all_gather(nlat_late, "sp", axis=0, tiled=True)

    length = sp * tokens
    cosine, sine = angles(length, ROPE)
    k_rope = rotate(rope_all.astype(f32), cosine, sine).astype(bf16)

    grads, dr = attend_backward(arrived, keyvals, k_rope, cosine, sine, heads)
    split = heads * WIDTH
    own_keys = heads * PLAIN_HEAD_WIDTH

    returned = lax.all_to_all(
        grads.reshape(sp, tokens, -1), "sp", split_axis=0, concat_axis=0, tiled=True
    )
    weight_part = lax.dot_general(
        grads[:, split:], nlat_all, (((0,), (0,)), ((), ())), preferred_element_type=f32
    ).astype(bf16)
    weight_part = weight_part.reshape(2, -1, channels)
    weight_sum = lax.psum_scatter(weight_part, "dp", scatter_dimension=1, tiled=True)
    weight_sum = lax.ppermute(weight_sum, ("sp", "dp"), to_holder)
    weight_grads = lax.all_gather(weight_sum, "sp", axis=1, tiled=True).astype(f32)

    rope_parts = rotate(dr, cosine, -sine).reshape(sp, -1, tokens)
    rope_parts = lax.all_to_all(rope_parts, "sp", split_axis=0, concat_axis=0, tiled=True)
    rope_grad = jnp.sum(rope_parts, axis=0).reshape(tokens, ROPE)

    query_grad = returned[:, :, :split].transpose(1, 0, 2).reshape(tokens, -1)
    dk = returned[:, :, split : split + own_keys].transpose(1, 0, 2).reshape(tokens, -1)
    dv = returned[:, :, split + own_keys :].transpose(1, 0, 2).reshape(tokens, -1)
    d_nlat = lax.dot_general(dk, whole[0], NN, preferred_element_type=f32)
    d_nlat = d_nlat + lax.dot_general(dv, whole[1], NN, preferred_element_type=f32)
    gain_grad = lax.psum(jnp.sum(d_nlat * normed, axis=0), ("sp", "dp"))
    scaled = d_nlat * latent_norm_gain
    latent_grad = inv_rms * (scaled - normed * jnp.mean(scaled * normed, axis=-1, keepdims=True))
    return (
        query_grad[None],
        latent_grad[None],
        rope_grad[None],
        weight_grads[0],
        weight_grads[1],
        gain_grad,
    )


def solution(mesh):
    in_specs = (
        P("dp", "sp", None),
        P("dp", "sp", None),
        P("dp", "sp", None),
        P(),
        P("dp", None),
        P("dp", None),
        P("dp", "sp", None),
    )
    out_specs = (
        P("dp", "sp", None),
        P("dp", "sp", None),
        P("dp", "sp", None),
        P("dp", None),
        P("dp", None),
        P(),
    )
    return jax.shard_map(local, mesh=mesh, in_specs=in_specs, out_specs=out_specs, check_vma=False)
```

```python
import functools
import math

import jax
import jax.numpy as jnp
from jax import lax
from jax.experimental import pallas as pl
from jax.experimental.pallas import tpu as pltpu
from jax.sharding import PartitionSpec as P

ATTENTION_HEADS = 32
PLAIN_HEAD_WIDTH = 64
ROPE = 32
VALUE_HEAD_WIDTH = 64
SPAN = 64
WIDTH = PLAIN_HEAD_WIDTH + ROPE

eps = 1e-06
rope_base = 10000.0


def rotate(values, cosine, sine):
    half = values.shape[-1] // 2
    first = values[..., :half]
    second = values[..., half:]
    return jnp.concatenate(
        [first * cosine - second * sine, second * cosine + first * sine], axis=-1
    )


def angles(positions, width):
    inverse = 1.0 / rope_base ** (jnp.arange(0, width, 2, dtype=jnp.float32) / width)
    turned = positions[:, None] * inverse[None, :]
    return (jnp.cos(turned), jnp.sin(turned))


NT = (((1,), (1,)), ((), ()))
NN = (((1,), (0,)), ((), ()))


def mm(a, b, dims=NN):
    return lax.dot_general(a, b, dims, preferred_element_type=jnp.float32)


def attention_kernel(
    heads, tile,
    arrived, keyvals, cosine, sine,
    grads_out, dr_out,
    q_s, go_s, k_s, kt_s, v_s, s_s, dp_s, dk_s, dv_s, dq_s,
):
    f32 = jnp.float32
    bf16 = jnp.bfloat16
    length = keyvals.shape[0]
    blocks = length // tile
    scale = WIDTH ** (-0.5)
    steep = scale * math.log2(math.e)
    half = ROPE // 2
    pid = pl.program_id(0)

    for h in range(heads):
        @pl.when(pid == h)
        def _():
            raw = arrived[:, h * WIDTH : (h + 1) * WIDTH]
            turned = rotate(
                raw[:, PLAIN_HEAD_WIDTH:].astype(f32), cosine[:, :half], sine[:, :half]
            ).astype(bf16)
            q_s[...] = jnp.concatenate([raw[:, :PLAIN_HEAD_WIDTH], turned], axis=1)
            base = heads * WIDTH + h * VALUE_HEAD_WIDTH
            go_s[...] = arrived[:, base : base + VALUE_HEAD_WIDTH]
            shared = heads * (PLAIN_HEAD_WIDTH + VALUE_HEAD_WIDTH)
            both = jnp.concatenate(
                [
                    keyvals[:, h * PLAIN_HEAD_WIDTH : (h + 1) * PLAIN_HEAD_WIDTH],
                    keyvals[:, shared : shared + ROPE],
                ],
                axis=1,
            )
            k_s[...] = both
            base = heads * PLAIN_HEAD_WIDTH + h * VALUE_HEAD_WIDTH
            v_s[...] = keyvals[:, base : base + VALUE_HEAD_WIDTH]

    for b in range(blocks):
        kt_s[b] = k_s[b * tile : (b + 1) * tile, :].astype(f32).T.astype(bf16)
    dk_s[...] = jnp.zeros_like(dk_s)
    dv_s[...] = jnp.zeros_like(dv_s)

    key_seg = lax.broadcasted_iota(jnp.int32, (tile, tile), 0) // SPAN
    query_seg = lax.broadcasted_iota(jnp.int32, (tile, tile), 1) // SPAN

    def fold(x, op):
        return op(x.reshape(tile // 8, 8, tile), axis=0)

    def query_block(qi, _):
        rows = pl.ds(pl.multiple_of(qi * tile, tile), tile)
        q = q_s[rows, :]
        go = go_s[rows, :]

        def score(kb, peak, diagonal=False):
            at = pl.ds(pl.multiple_of(kb * tile, tile), tile)
            s = mm(k_s[at, :], q, NT)
            if diagonal:
                s = jnp.where(key_seg <= query_seg, s, -1e30)
            s_s[at, :] = s
            dp_s[at, :] = mm(v_s[at, :], go, NT)
            return jnp.maximum(peak, fold(s, jnp.max))

        peak = lax.fori_loop(0, qi, score, jnp.full((8, tile), -1e30, f32))
        peak = score(qi, peak, diagonal=True)
        top = jnp.max(peak, axis=0, keepdims=True) * steep

        def weigh(kb, carry):
            total, mixed = carry
            at = pl.ds(pl.multiple_of(kb * tile, tile), tile)
            p = jnp.exp2(s_s[at, :] * steep - top)
            s_s[at, :] = p
            return total + fold(p, jnp.sum), mixed + fold(p * dp_s[at, :], jnp.sum)

        zero = jnp.zeros((8, tile), f32)
        total, mixed = lax.fori_loop(0, qi + 1, weigh, (zero, zero))
        inverse = 1.0 / jnp.sum(total, axis=0, keepdims=True)
        delta = jnp.sum(mixed, axis=0, keepdims=True) * inverse

        dq_s[...] = jnp.zeros_like(dq_s)

        def spread(kb, _):
            at = pl.ds(pl.multiple_of(kb * tile, tile), tile)
            probs = s_s[at, :] * inverse
            ds = (probs * (dp_s[at, :] - delta)).astype(bf16)
            dv_s[at, :] += mm(probs.astype(bf16), go)
            dk_s[at, :] += mm(ds, q)
            dq_s[...] += mm(kt_s[kb], ds)
            return 0

        lax.fori_loop(0, qi + 1, spread, 0)
        dq = dq_s[...].T * scale
        back = rotate(dq[:, PLAIN_HEAD_WIDTH:], cosine[rows, :half], -sine[rows, :half])
        done = jnp.concatenate([dq[:, :PLAIN_HEAD_WIDTH], back], axis=1).astype(bf16)
        for h in range(heads):
            @pl.when(pid == h)
            def _():
                grads_out[rows, h * WIDTH : (h + 1) * WIDTH] = done
        return 0

    lax.fori_loop(0, blocks, query_block, 0)

    dk = dk_s[...] * scale
    for h in range(heads):
        @pl.when(pid == h)
        def _():
            base = heads * WIDTH + h * PLAIN_HEAD_WIDTH
            grads_out[:, base : base + PLAIN_HEAD_WIDTH] = dk[:, :PLAIN_HEAD_WIDTH].astype(bf16)
            base = heads * (WIDTH + PLAIN_HEAD_WIDTH) + h * VALUE_HEAD_WIDTH
            grads_out[:, base : base + VALUE_HEAD_WIDTH] = dv_s[...].astype(bf16)
            if h == 0:
                dr_out[...] = dk[:, PLAIN_HEAD_WIDTH:]
            else:
                dr_out[...] += dk[:, PLAIN_HEAD_WIDTH:]


def attend_backward(arrived, keyvals, cosine, sine, heads):
    length = arrived.shape[0]
    tile = 256
    f32 = jnp.float32
    bf16 = jnp.bfloat16

    def whole(a):
        return pl.BlockSpec(a.shape, lambda i: (0,) * len(a.shape))

    outs = (
        jax.ShapeDtypeStruct((length, heads * (WIDTH + PLAIN_HEAD_WIDTH + VALUE_HEAD_WIDTH)), bf16),
        jax.ShapeDtypeStruct((length, ROPE), f32),
    )
    ins = (arrived, keyvals, cosine, sine)
    return pl.pallas_call(
        functools.partial(attention_kernel, heads, tile),
        grid=(heads,),
        out_shape=outs,
        in_specs=[whole(a) for a in ins],
        out_specs=tuple(whole(a) for a in outs),
        scratch_shapes=[
            pltpu.VMEM((length, WIDTH), bf16),
            pltpu.VMEM((length, VALUE_HEAD_WIDTH), bf16),
            pltpu.VMEM((length, WIDTH), bf16),
            pltpu.VMEM((length // tile, WIDTH, tile), bf16),
            pltpu.VMEM((length, VALUE_HEAD_WIDTH), bf16),
            pltpu.VMEM((length, tile), f32),
            pltpu.VMEM((length, tile), f32),
            pltpu.VMEM((length, WIDTH), f32),
            pltpu.VMEM((length, VALUE_HEAD_WIDTH), f32),
            pltpu.VMEM((WIDTH, tile), f32),
        ],
        compiler_params=pltpu.CompilerParams(
            dimension_semantics=("arbitrary",), vmem_limit_bytes=56 * 1024 * 1024
        ),
        cost_estimate=pl.CostEstimate(
            flops=heads * length * length * 420, bytes_accessed=8 * length * 1024,
            transcendentals=heads * length * length // 2,
        ),
    )(*ins)


def ring_kernel(n, block, out, send, recv, own):
    half = n // 2
    me = lax.axis_index("sp")
    odd = me % 2
    place = (1 - odd) * (me // 2) + odd * (n - 1 - me // 2)

    def device(p):
        back = p // half
        return (1 - back) * (2 * p) + back * (2 * (n - 1 - p) + 1)

    right = device((place + 1) % n)
    left = device((place + n - 1) % n)
    barrier = pltpu.get_barrier_semaphore()
    for other in (left, right):
        pl.semaphore_signal(
            barrier, inc=1, device_id={"sp": other}, device_id_type=pl.DeviceIdType.MESH
        )
    pl.semaphore_wait(barrier, 2)
    kept = [
        pltpu.make_async_copy(block.at[way], out.at[way, me], own.at[way]) for way in range(2)
    ]
    for copy in kept:
        copy.start()
    for step in range(n - 1):
        copies = []
        for way, target in ((0, right), (1, left)):
            slot = device((place + n - step) % n if way == 0 else (place + step) % n)
            source = block.at[way] if step == 0 else out.at[way, slot]
            copies.append(
                pltpu.make_async_remote_copy(
                    src_ref=source,
                    dst_ref=out.at[way, slot],
                    send_sem=send.at[way, step],
                    recv_sem=recv.at[way, step],
                    device_id={"sp": target},
                    device_id_type=pl.DeviceIdType.MESH,
                )
            )
        for copy in copies:
            copy.start()
        for copy in copies:
            copy.wait()
    for copy in kept:
        copy.wait()


def ring_gather(block, n):
    rows, channels = block.shape[1:]
    gathered = pl.pallas_call(
        functools.partial(ring_kernel, n),
        out_shape=jax.ShapeDtypeStruct((2, n, rows, channels), block.dtype),
        in_specs=[pl.BlockSpec(memory_space=pltpu.VMEM)],
        out_specs=pl.BlockSpec(memory_space=pltpu.VMEM),
        scratch_shapes=[
            pltpu.SemaphoreType.DMA((2, n - 1)),
            pltpu.SemaphoreType.DMA((2, n - 1)),
            pltpu.SemaphoreType.DMA((2,)),
        ],
        compiler_params=pltpu.CompilerParams(
            collective_id=0, has_side_effects=True, vmem_limit_bytes=16 * 1024 * 1024
        ),
    )(block)
    return gathered.reshape(2, n * rows, channels)


def normalise(latent):
    lat = latent.astype(jnp.float32)
    inv_rms = lax.rsqrt(jnp.mean(lat * lat, axis=-1, keepdims=True) + eps)
    return lat * inv_rms, inv_rms


def local(query, latent, rope_key, latent_norm_gain, key_up_matrix, value_up_matrix, out_grad):
    f32 = jnp.float32
    bf16 = jnp.bfloat16
    sp = lax.axis_size("sp")
    dp = lax.axis_size("dp")
    tokens, channels = latent.shape[1:]
    heads = ATTENTION_HEADS // sp
    ratio = sp // dp
    to_user = [
        (s * dp + d, (d * ratio + s // dp) * dp + s % dp) for s in range(sp) for d in range(dp)
    ]
    to_holder = [(b, a) for a, b in to_user]

    stacked = jnp.stack([key_up_matrix, value_up_matrix])
    whole = lax.all_gather(stacked, "dp", axis=1, tiled=True)
    packed = jnp.concatenate(
        [
            query[0].reshape(tokens, sp, heads * WIDTH),
            out_grad[0].reshape(tokens, sp, heads * VALUE_HEAD_WIDTH),
        ],
        axis=-1,
    ).transpose(1, 0, 2)
    arrived = lax.all_to_all(packed, "sp", split_axis=0, concat_axis=0, tiled=True)
    arrived = arrived.reshape(sp * tokens, -1)

    normed, inv_rms = normalise(latent[0])
    nlat = (normed * latent_norm_gain).astype(bf16)
    key_cols = lax.dot_general(nlat, whole[0], NT, preferred_element_type=f32).astype(bf16)
    value_cols = lax.dot_general(nlat, whole[1], NT, preferred_element_type=f32).astype(bf16)
    at = (lax.axis_index("sp") * tokens + jnp.arange(tokens)).astype(f32)
    near_cosine, near_sine = angles(at, ROPE)
    k_rope = rotate(rope_key[0].astype(f32), near_cosine, near_sine).astype(bf16)
    keyvals = jnp.concatenate(
        [
            key_cols.reshape(tokens, sp, heads * PLAIN_HEAD_WIDTH),
            value_cols.reshape(tokens, sp, heads * VALUE_HEAD_WIDTH),
            jnp.broadcast_to(k_rope[:, None, :], (tokens, sp, ROPE)),
        ],
        axis=-1,
    ).transpose(1, 0, 2)
    keyvals = lax.all_to_all(keyvals, "sp", split_axis=0, concat_axis=0, tiled=True)
    keyvals = keyvals.reshape(sp * tokens, -1)

    nlat_late, whole = lax.optimization_barrier((nlat, whole))
    nlat_all = lax.all_gather(nlat_late, "sp", axis=0, tiled=True)

    length = sp * tokens
    cosine, sine = angles(jnp.arange(length, dtype=f32), ROPE)

    grads, dr = attend_backward(arrived, keyvals, cosine, sine, heads)
    split = heads * WIDTH
    own_keys = heads * PLAIN_HEAD_WIDTH

    returned = lax.all_to_all(
        grads.reshape(sp, tokens, -1), "sp", split_axis=0, concat_axis=0, tiled=True
    )
    weight_part = lax.dot_general(
        grads[:, split:], nlat_all, (((0,), (0,)), ((), ())), preferred_element_type=f32
    ).astype(bf16)
    weight_part = weight_part.reshape(2, -1, channels)
    weight_sum = lax.psum_scatter(weight_part, "dp", scatter_dimension=1, tiled=True)
    weight_sum = lax.ppermute(weight_sum, ("sp", "dp"), to_holder)
    gathered = ring_gather(weight_sum, sp)

    dr, _ = lax.optimization_barrier((dr, weight_part))
    rope_parts = rotate(dr, cosine, -sine).reshape(sp, -1, tokens)
    gathered, returned, rope_parts = lax.optimization_barrier((gathered, returned, rope_parts))
    weight_grads = gathered.astype(f32)
    rope_parts = lax.all_to_all(rope_parts, "sp", split_axis=0, concat_axis=0, tiled=True)
    rope_grad = jnp.sum(rope_parts, axis=0).reshape(tokens, ROPE)

    query_grad = returned[:, :, :split].transpose(1, 0, 2).reshape(tokens, -1)
    dk = returned[:, :, split : split + own_keys].transpose(1, 0, 2).reshape(tokens, -1)
    dv = returned[:, :, split + own_keys :].transpose(1, 0, 2).reshape(tokens, -1)
    d_nlat = lax.dot_general(dk, whole[0], NN, preferred_element_type=f32)
    d_nlat = d_nlat + lax.dot_general(dv, whole[1], NN, preferred_element_type=f32)
    gain_grad = lax.psum(jnp.sum(d_nlat * normed, axis=0), ("sp", "dp"))
    scaled = d_nlat * latent_norm_gain
    latent_grad = inv_rms * (scaled - normed * jnp.mean(scaled * normed, axis=-1, keepdims=True))
    return (
        query_grad[None],
        latent_grad[None],
        rope_grad[None],
        weight_grads[0],
        weight_grads[1],
        gain_grad,
    )


def solution(mesh):
    in_specs = (
        P("dp", "sp", None),
        P("dp", "sp", None),
        P("dp", "sp", None),
        P(),
        P("dp", None),
        P("dp", None),
        P("dp", "sp", None),
    )
    out_specs = (
        P("dp", "sp", None),
        P("dp", "sp", None),
        P("dp", "sp", None),
        P("dp", None),
        P("dp", None),
        P(),
    )
    return jax.shard_map(local, mesh=mesh, in_specs=in_specs, out_specs=out_specs, check_vma=False)
```
